32 devices in a mesh: gr: 2 (over core), fs: 8 (over z, y), tp: 2 (over x).
Axes of the slice: x: 2, y: 2, z: 4, core: 2. Of those that a mesh axis runs over, the one named last changes fastest.
Arguments:
- tokens: bfloat16 [6144, 2048], P(('gr', 'fs')), may hold values from -6 to 6
- route_ids: int32 [6144, 2], P(('gr', 'fs')), may hold values from 0 to 7, as said below
- route_weights: float32 [6144, 2], P(('gr', 'fs')), may hold values from 0.1 to 1
- norm_gain: float32 [2048], P(('gr', 'fs')), may hold values from 0.1 to 1.9
- gate_weight: float32 [8, 2048, 1024], P(None, ('gr', 'fs'), 'tp'), may hold values from -0.125 to 0.125
- up_weight: float32 [8, 2048, 1024], P(None, ('gr', 'fs'), 'tp'), may hold values from -0.125 to 0.125
- down_weight: float32 [8, 1024, 2048], P(None, ('gr', 'fs'), 'tp'), may hold values from -0.1875 to 0.1875
Outputs:
- gate_new: bfloat16 [8, 2048, 1024], P('fs', None, 'tp')
- up_new: bfloat16 [8, 2048, 1024], P('fs', None, 'tp')
- down_new: bfloat16 [8, 1024, 2048], P('fs', 'tp')
- mixed: bfloat16 [6144, 2048], P(('gr', 'fs'), 'tp')
The draws below stay inside these ranges and needn't reach their ends.
Inputs may be any that keep to these rules, and one draw needn't show every extreme that they name: `route_ids`: each row names two different experts of one group (expert e belongs to group e // 2); in each device's block of 384 rows every expert is named by exactly 96 rows.
All inputs are finite; a program needn't handle non-finite values.
Results may differ from the reference program's by a relative error of at most 0.015.
Values may be sent and summed in bfloat16 or wider, within the bound.
No kernel may reach another device: no remote copies, remote signals or barrier semaphores. Data moves between devices by JAX's collectives and lax.ppermute only.
A program may use at most 64 MiB of HBM per device.

```python
import jax
import jax.numpy as jnp
from jax import lax

D = 2048
FF = 1024
GROUPS = 4
TOK_DEV = 384
EXPERTS = 8
EPG = 2
HID_DEV = 512
TOKENS = 6144
N_GR = 2
N_FS = 8


def draw_route_ids(key, part):
    blocks = N_GR * N_FS

    def one_block(block_key):
        key_order, key_first, key_step = jax.random.split(block_key, 3)
        place = jax.random.permutation(key_order, TOK_DEV).astype(jnp.int32)
        group = place % GROUPS
        inner = place // GROUPS
        first_shift = jax.random.randint(key_first, (GROUPS,), 0, EPG).astype(jnp.int32)
        step_shift = jax.random.randint(key_step, (GROUPS,), 0, EPG - 1).astype(jnp.int32)
        first = (inner + first_shift[group]) % EPG
        stride = 1 + (inner // EPG + step_shift[group]) % (EPG - 1)
        second = (first + stride) % EPG
        return jnp.stack([group * EPG + first, group * EPG + second], axis=1).astype(jnp.int32)
    keys = jax.random.split(key, blocks)
    return jax.vmap(one_block)(keys).reshape(TOKENS, 2)


def shard_levels(stream_key, shape, cuts, low, top_value):
    gain, own = 1.0, jax.random.fold_in(stream_key, 6)
    for position, shards_of in cuts:
        draws = jnp.exp(jax.random.uniform(jax.random.fold_in(own, position), (shards_of,), jnp.float32, low / len(cuts), top_value / len(cuts)))
        gain = gain * jnp.repeat(draws, shape[position] // shards_of).reshape([-1 if axis == position else 1 for axis in range(len(shape))])
    return gain


def gaussian(own_key, shape, width, limit, cuts=(), held_as=jnp.bfloat16):
    level = shard_levels(own_key, shape, cuts, -0.22, 0.18) if cuts else 1.0
    array = jax.random.normal(own_key, shape, jnp.float32) * width * level
    return jnp.minimum(jnp.maximum(array, -limit), limit).astype(held_as)


def setup_inputs(seed: int = 0) -> dict:
    arg_keys = jax.random.split(jax.random.key(seed), 8)
    return {
        "tokens": gaussian(arg_keys[0], (TOKENS, D), 1.0, 6.0, ((0, 16),)),
        "route_ids": draw_route_ids(jax.random.fold_in(arg_keys[7], 71), 0),
        "route_weights": jnp.clip(0.1 + 0.9 * jax.random.uniform(arg_keys[2], (TOKENS, 2), jnp.float32) ** shard_levels(arg_keys[2], (TOKENS, 2), ((0, 16),), -0.2, 0.2), 0.1, 1.0),
        "norm_gain": jnp.clip(1.0 + 0.18 * jax.random.normal(arg_keys[3], (D,), jnp.float32), 0.1, 1.9),
        "gate_weight": gaussian(arg_keys[4], (EXPERTS, D, FF), D ** -0.5, 0.125, ((1, 16), (2, 2)), jnp.float32),
        "up_weight": gaussian(arg_keys[5], (EXPERTS, D, FF), D ** -0.5, 0.125, ((1, 16), (2, 2)), jnp.float32),
        "down_weight": gaussian(arg_keys[6], (EXPERTS, FF, D), FF ** -0.5, 0.1875, ((1, 16), (2, 2)), jnp.float32),
    }


def expert_block(args):
    gate_one, up_one, down_one, rows = args
    first = jnp.dot(rows, gate_one, preferred_element_type=jnp.float32)
    second = jnp.dot(rows, up_one, preferred_element_type=jnp.float32)
    hidden = (jax.nn.silu(first) * second).astype(jnp.bfloat16)
    count = rows.shape[0]
    pieces = hidden.reshape(count, FF // HID_DEV, HID_DEV).astype(jnp.float32)
    down_pieces = down_one.reshape(FF // HID_DEV, HID_DEV, D).astype(jnp.float32)
    partials = jnp.einsum('mbf,bfd->bmd', pieces, down_pieces).astype(jnp.bfloat16)
    return lax.optimization_barrier(jnp.sum(partials.astype(jnp.float32), axis=0)).astype(jnp.bfloat16)

def reference(tokens, route_ids, route_weights, norm_gain, gate_weight, up_weight, down_weight):
    gate_new = (gate_weight * norm_gain[None, :, None]).astype(jnp.bfloat16)
    up_new = (up_weight * norm_gain[None, :, None]).astype(jnp.bfloat16)
    down_new = down_weight.astype(jnp.bfloat16)
    widened = tokens.astype(jnp.float32)
    normed = (widened * lax.rsqrt(lax.optimization_barrier(jnp.mean(widened * widened, axis=-1, keepdims=True)) + 1e-06)).astype(jnp.bfloat16)
    flat_ids = route_ids.reshape(-1)
    per_expert = flat_ids.shape[0] // EXPERTS
    order = jnp.argsort(flat_ids, stable=True).astype(jnp.int32).reshape(EXPERTS, per_expert)

    def one_expert(args):
        gate_one, up_one, down_one, picks = args
        rows = normed[picks // 2]
        return expert_block((gate_one, up_one, down_one, rows))
    results = lax.map(one_expert, (gate_new, up_new, down_new, order))
    route_out = jnp.zeros((flat_ids.shape[0], D), jnp.bfloat16).at[order.reshape(-1)].set(results.reshape(-1, D))
    route_out = route_out.reshape(-1, 2, D).astype(jnp.float32)
    mixed = lax.optimization_barrier(jnp.sum(route_weights[:, :, None] * route_out, axis=1)).astype(jnp.bfloat16)
    return (gate_new, up_new, down_new, mixed)
```

```python
import jax
import jax.numpy as jnp
from jax import lax
from jax.sharding import PartitionSpec as P

GROUPS = 4
BF16 = jnp.bfloat16
F32 = jnp.float32


def exchange(x, axes, pairs):
    return lax.ppermute(x, axes, pairs)


def ordered(index, mine, other, axis):
    return jnp.where(
        index == 0,
        jnp.concatenate([mine, other], axis=axis),
        jnp.concatenate([other, mine], axis=axis),
    )


def normalise(tokens):
    widened = tokens.astype(F32)
    return (
        widened * lax.rsqrt(jnp.mean(widened * widened, axis=-1, keepdims=True) + 1e-06)
    ).astype(BF16)


def general(tokens, route_ids, route_weights, norm_gain, gate_weight, up_weight, down_weight):
    gate_folded = (gate_weight * norm_gain[None, :, None]).astype(BF16)
    up_folded = (up_weight * norm_gain[None, :, None]).astype(BF16)
    down_rounded = down_weight.astype(BF16)
    whole = [
        lax.all_gather(
            lax.all_to_all(w, "fs", split_axis=0, concat_axis=1, tiled=True),
            "gr", axis=1, tiled=True,
        )
        for w in (gate_folded, up_folded, down_rounded)
    ]
    gate_new, up_new = whole[0], whole[1]
    down_new = lax.all_to_all(whole[2], "tp", split_axis=1, concat_axis=2, tiled=True)
    tok, width = tokens.shape
    experts = gate_weight.shape[0]
    cap = 2 * tok // experts
    flat_ids = route_ids.reshape(-1)
    onehot = (flat_ids[:, None] == jnp.arange(experts, dtype=jnp.int32)[None, :]).astype(jnp.int32)
    slot = jnp.sum(jnp.cumsum(onehot, axis=0) * onehot, axis=1) - 1
    position = flat_ids * cap + slot
    source = (
        jnp.zeros((experts * cap,), jnp.int32)
        .at[position]
        .set(jnp.arange(2 * tok, dtype=jnp.int32) // 2)
    )
    outgoing = normalise(tokens)[source].reshape(experts, cap, width)
    received = lax.all_to_all(outgoing, "fs", split_axis=0, concat_axis=0, tiled=True)
    senders, count, _ = received.shape
    rows = received.reshape(senders * count, width)
    first = jnp.dot(rows, gate_new[0], preferred_element_type=F32)
    second = jnp.dot(rows, up_new[0], preferred_element_type=F32)
    hidden = (jax.nn.silu(first) * second).astype(BF16)
    partial_out = jnp.dot(hidden, down_new[0], preferred_element_type=F32)
    summed = lax.psum_scatter(
        partial_out.reshape(senders, count, width).astype(BF16),
        "tp", scatter_dimension=2, tiled=True,
    )
    returned = lax.all_to_all(summed, "fs", split_axis=0, concat_axis=0, tiled=True)
    columns = returned.shape[2]
    route_out = returned.reshape(experts * cap, columns)[position].reshape(tok, 2, columns)
    mixed = jnp.sum(route_weights[:, :, None] * route_out.astype(F32), axis=1).astype(BF16)
    return (gate_new, up_new, down_new, mixed)


def paired(tokens, route_ids, route_weights, norm_gain, gate_weight, up_weight, down_weight):
    experts, depth, hid = gate_weight.shape
    tok, width = tokens.shape
    share = down_weight.shape[1]
    cols = down_weight.shape[2]
    cap = tok // GROUPS
    gr, fs, tp = lax.axis_index("gr"), lax.axis_index("fs"), lax.axis_index("tp")
    group, member = fs // 2, fs % 2
    swap = [(0, 1), (1, 0)]
    across = [(f, f ^ 1) for f in range(experts)]

    def shift(k):
        return [(f, (f // 2 + k) % GROUPS * 2 + f % 2) for f in range(experts)]

    gain = norm_gain[None, :, None]
    both = jnp.concatenate(
        [(gate_weight * gain).astype(BF16), (up_weight * gain).astype(BF16)], axis=1
    )
    both = lax.all_to_all(both, "fs", split_axis=0, concat_axis=0, tiled=True)

    of_group = route_ids[:, 0] // 2
    ahead = (of_group - group) % GROUPS
    onehot = (ahead[None, :] == jnp.arange(GROUPS, dtype=jnp.int32)[:, None])
    token = jnp.arange(tok, dtype=jnp.int32)
    upto = (token[:, None] <= token[None, :]).astype(BF16)
    rank = jnp.dot(onehot.astype(BF16), upto, preferred_element_type=F32)
    rank = jnp.sum(jnp.where(onehot, rank, 0.0), axis=0).astype(jnp.int32) - 1
    position = ahead * cap + rank
    placing = (token[:, None] == position[None, :]).astype(BF16)

    normed = lax.dynamic_slice_in_dim(normalise(tokens), tp * cols, cols, axis=1)
    sorted_rows = jnp.dot(placing, normed, preferred_element_type=F32).astype(BF16)
    is_first = route_ids[:, 0] % 2 == 0
    weights = jnp.stack(
        [
            jnp.where(is_first, route_weights[:, 0], route_weights[:, 1]),
            jnp.where(is_first, route_weights[:, 1], route_weights[:, 0]),
        ]
    )
    coarse = weights.astype(BF16)
    fine = (weights - coarse.astype(F32)).astype(BF16)
    parts = jnp.concatenate([coarse, fine], axis=0)
    sorted_weights = lax.dot_general(
        parts, placing, (((1,), (1,)), ((), ())), preferred_element_type=F32
    ).astype(BF16)
    extra = jnp.transpose(sorted_weights.reshape(4, GROUPS, cap), (1, 0, 2))
    extra = jnp.pad(extra, ((0, 0), (0, 4), (0, cols - cap)))
    outgoing = jnp.concatenate([sorted_rows.reshape(GROUPS, cap, cols), extra], axis=1)

    arrived = [outgoing[0]] + [exchange(outgoing[k], "fs", shift(k)) for k in range(1, GROUPS)]
    here = jnp.stack(arrived)
    half = GROUPS // 2
    here_x = exchange(here, "tp", swap)
    there = exchange(here, "fs", across)
    there_x = jnp.concatenate(
        [exchange(here_x[:half], "fs", across), exchange(there[half:], "tp", swap)], axis=0
    )
    rows = jnp.concatenate(
        [
            ordered(tp, here[:, :cap], here_x[:, :cap], 2),
            ordered(tp, there[:, :cap], there_x[:, :cap], 2),
        ],
        axis=0,
    ).reshape(2 * tok, width)
    scales = jnp.concatenate([here[:, cap:, :cap], there[:, cap:, :cap]], axis=0).astype(F32)
    scales = jnp.where(member == 0, scales[:, 0] + scales[:, 2], scales[:, 1] + scales[:, 3])
    scales = scales.reshape(2 * tok, 1)

    down_mine = lax.all_to_all(
        down_weight.astype(BF16), "fs", split_axis=0, concat_axis=0, tiled=True
    ).reshape(experts * share, cols)

    other = exchange(both, "gr", swap)
    gate_new = ordered(
        gr,
        both[:, :depth].reshape(experts * depth, hid),
        other[:, :depth].reshape(experts * depth, hid),
        0,
    )
    up_new = ordered(
        gr,
        both[:, depth:].reshape(experts * depth, hid),
        other[:, depth:].reshape(experts * depth, hid),
        0,
    )
    first = jnp.dot(rows, gate_new, preferred_element_type=F32)
    second = jnp.dot(rows, up_new, preferred_element_type=F32)
    hidden = (jax.nn.silu(first) * second).astype(BF16)
    hidden_x = exchange(hidden, "tp", swap)

    down_other = exchange(down_mine, "gr", swap)
    same = gr == tp
    out = jnp.dot(
        jnp.where(same, hidden, hidden_x), down_mine, preferred_element_type=F32
    ) + jnp.dot(jnp.where(same, hidden_x, hidden), down_other, preferred_element_type=F32)
    out = (out * scales).astype(BF16)
    from_pair = exchange(out[tok:], "fs", across)
    summed = (out[:tok].astype(F32) + from_pair.astype(F32)).astype(BF16)
    summed = summed.reshape(GROUPS, cap, cols)
    home = jnp.concatenate(
        [summed[0]] + [exchange(summed[k], "fs", shift(-k)) for k in range(1, GROUPS)], axis=0
    )
    mixed = lax.dot_general(
        placing, home, (((0,), (0,)), ((), ())), preferred_element_type=F32
    ).astype(BF16)

    crossed = lax.ppermute(down_mine, ("gr", "tp"), [(1, 2), (2, 1)])
    down_half = jnp.where(same, down_mine, crossed)
    down_new = ordered(gr, down_half, exchange(down_half, "gr", swap), 1)
    return (gate_new[None], up_new[None], down_new[None], mixed)


def solution(mesh):
    placed = (
        P(("gr", "fs"), None),
        P(("gr", "fs"), None),
        P(("gr", "fs"), None),
        P(("gr", "fs")),
        P(None, ("gr", "fs"), "tp"),
        P(None, ("gr", "fs"), "tp"),
        P(None, ("gr", "fs"), "tp"),
    )
    sizes = mesh.shape
    fits = sizes["gr"] == 2 and sizes["tp"] == 2 and sizes["fs"] == 2 * GROUPS
    return jax.shard_map(
        paired if fits else general,
        mesh=mesh,
        in_specs=placed,
        out_specs=(
            P("fs", None, "tp"),
            P("fs", None, "tp"),
            P("fs", "tp", None),
            P(("gr", "fs"), "tp"),
        ),
        check_vma=False,
    )
```
